32 devices in a mesh: sp: 16 (over z, y, x), tp: 2 (over core).
Axes of the slice: x: 2, y: 2, z: 4, core: 2. Of those that a mesh axis runs over, the one named last changes fastest.
Arguments:
- queries: bfloat16 [4096, 8, 128], P('sp', 'tp'), may hold values from -6 to 6
- keys: bfloat16 [4096, 2, 128], P('sp'), may hold values from -6 to 6
- values: bfloat16 [4096, 2, 128], P('sp'), may hold values from -6 to 6
- documents: int32 [4096], P('sp'), may hold values from 0 to 3, never falling along the last dimension, each value on 1 to 2304 neighbouring positions
- query_gain: float32 [128], replicated, may hold values from 0.25 to 4
- key_gain: float32 [128], replicated, may hold values from 0.25 to 4
- out_weight: bfloat16 [1024, 2048], P('tp'), may hold values from -0.1875 to 0.1875
- residual: bfloat16 [4096, 2048], P('sp'), may hold values from -6 to 6
- norm_gain: float32 [2048], replicated, may hold values from 0.1 to 1.9
- up_weight: bfloat16 [2048, 6144], P('sp', 'tp'), may hold values from -0.125 to 0.125
- down_weight: bfloat16 [2048, 6144], P('sp', 'tp'), may hold values from -0.078125 to 0.078125
Outputs:
- layer_out: bfloat16 [4096, 2048], P(('sp', 'tp'))
The draws below stay inside these ranges and needn't reach their ends.
Inputs may be any that keep to these rules, and one draw needn't show every extreme that they name: `documents`: document numbers never fall along the sequence; one document covers exactly (9) * 256 positions.
All inputs are finite; a program needn't handle non-finite values.
Results may differ from the reference program's by a relative error of at most 0.017.
Values may be sent and summed in bfloat16 or wider, within the bound.
A program may use at most 128 MiB of HBM per device.

```python
import math
import jax
import jax.numpy as jnp
import numpy as np
from jax import lax

D = 2048
QUERY_HEADS = 8
KEY_VALUE_HEADS = 2
HEAD_SIZE = 128
FF = 6144
GRID = 64
TOKENS_PER_SHARD = 256
PACKED_TOKENS = 4096
N_SP = 16
N_TP = 2


def group_shared_keys(key):
    return jax.random.truncated_normal(jax.random.fold_in(key, 31), -6.0, 6.0, (PACKED_TOKENS, KEY_VALUE_HEADS, HEAD_SIZE), jnp.float32)


def draw_keys(key, part):
    return group_shared_keys(key).astype(jnp.bfloat16)


def draw_queries(key, part):
    fresh = jax.random.truncated_normal(jax.random.fold_in(key, 37), -6.0, 6.0, (PACKED_TOKENS, QUERY_HEADS, HEAD_SIZE), jnp.float32)
    return fresh.astype(jnp.bfloat16)


def draw_query_gain(key, part):
    return 1.0 + 0.18 * jax.random.truncated_normal(jax.random.fold_in(key, 43), -4.0, 4.0, (HEAD_SIZE,), jnp.float32)


def draw_key_gain(key, part):
    return 1.0 + 0.18 * jax.random.truncated_normal(jax.random.fold_in(key, 53), -4.0, 4.0, (HEAD_SIZE,), jnp.float32)


def level_of(own_key, shape, shards, least, high):
    factor_of = 1.0
    for axis_at, blocks in shards:
        steps = jax.random.uniform(jax.random.fold_in(jax.random.fold_in(own_key, 6), axis_at), (blocks,), jnp.float32, least / len(shards), high / len(shards))
        factor_of = factor_of * jnp.repeat(jnp.exp(steps), shape[axis_at] // blocks).reshape((-1,) + (1,) * (len(shape) - 1 - axis_at))
    return factor_of


def profile(number_of, total, bound, slope):
    weights = [(1 << 20) // math.isqrt(standing ** slope) + 1 for standing in range(2, number_of + 1)]
    surplus, holding = total - bound - (number_of - 1), [1] * (number_of - 1)
    while surplus > 0:
        candidates = [i for i in range(number_of - 1) if holding[i] < bound]
        mass, budget = sum([weights[i] for i in candidates]), surplus
        for i in candidates:
            addition = min(bound - holding[i], max(1, budget * weights[i] // mass), surplus)
            holding[i] = holding[i] + addition
            surplus = surplus - addition
    return np.array([bound] + holding)


def uneven_parts(key, amount, total, most, lean):
    if amount == 2:
        one = jax.random.randint(key, (), max(1, total - most), min(most, total - 1) + 1)
        return jnp.stack([one, total - one])
    lengths = jnp.asarray(profile(amount, total, most, lean), jnp.int32)
    twos = (amount - 1) // 2
    source_of, taker = lengths[1:1 + 2 * twos:2], lengths[2:2 + 2 * twos:2]
    slack = jnp.minimum(source_of - 1, most - taker)
    shifted = jax.random.randint(jax.random.fold_in(key, 1), (twos,), 0, 1 << 20) % (slack + 1)
    lengths = lengths.at[1:1 + 2 * twos:2].set(source_of - shifted).at[2:2 + 2 * twos:2].set(taker + shifted)
    return lengths[jax.random.permutation(jax.random.fold_in(key, 2), amount)]


def scatter_about(rng, shape, scale, limit, split=(), kind=jnp.bfloat16):
    drawn = jax.random.normal(rng, shape, jnp.float32) * scale
    if len(split) > 0:
        drawn = level_of(rng, shape, split, -0.22, 0.18) * drawn
    return jnp.clip(drawn, min=-limit, max=limit).astype(kind)


def setup_inputs(seed: int = 0) -> dict:
    key_of = jax.random.split(jax.random.key(seed), 12)
    return {
        "queries": draw_queries(jax.random.fold_in(key_of[11], 71), 0),
        "keys": draw_keys(jax.random.fold_in(key_of[11], 71), 0),
        "values": scatter_about(key_of[2], (PACKED_TOKENS, KEY_VALUE_HEADS, HEAD_SIZE), 1.0, 6.0, ((0, 16),)),
        "documents": jnp.searchsorted(jnp.cumsum(uneven_parts(key_of[3], N_SP // 4, PACKED_TOKENS, (N_SP // 2 + 1) * TOKENS_PER_SHARD, 0)), jnp.arange(PACKED_TOKENS), side="right").astype(jnp.int32),
        "query_gain": draw_query_gain(jax.random.fold_in(key_of[11], 71), 0),
        "key_gain": draw_key_gain(jax.random.fold_in(key_of[11], 71), 0),
        "out_weight": scatter_about(key_of[6], (QUERY_HEADS * HEAD_SIZE, D), (QUERY_HEADS * HEAD_SIZE) ** -0.5, 0.1875, ((0, 2),)),
        "residual": scatter_about(key_of[7], (PACKED_TOKENS, D), 1.0, 6.0, ((0, 16),)),
        "norm_gain": jnp.clip(1.0 + 0.18 * jax.random.normal(key_of[8], (D,), jnp.float32), 0.1, 1.9),
        "up_weight": scatter_about(key_of[9], (D, FF), D ** -0.5, 0.125, ((0, 16), (1, 2))),
        "down_weight": scatter_about(key_of[10], (D, FF), FF ** -0.5, 0.078125, ((0, 16), (1, 2))),
    }


EPS = 1e-06
THETA = 10000.0

def head_norm(block, gain):
    return block * lax.rsqrt(lax.optimization_barrier(jnp.mean(block * block, axis=-1, keepdims=True)) + EPS) * gain

def rotate(block, positions):
    head_width = block.shape[-1]
    pair_count = head_width // 4
    inverse = THETA ** (-jnp.arange(pair_count, dtype=jnp.float32) / pair_count)
    grid_row = (positions // GRID).astype(jnp.float32)[:, None] * inverse
    grid_col = (positions % GRID).astype(jnp.float32)[:, None] * inverse
    angles = jnp.concatenate([grid_row, grid_row, grid_col, grid_col], axis=-1)
    cosine = jnp.cos(angles)[:, None, :]
    sine_table = jnp.sin(angles)[:, None, :]
    turned = jnp.concatenate([-block[..., pair_count:2 * pair_count], block[..., 0:pair_count], -block[..., 3 * pair_count:], block[..., 2 * pair_count:3 * pair_count]], axis=-1)
    return block * cosine + turned * sine_table

def channel_norm(rows_in, gain):
    widened = rows_in.astype(jnp.float32)
    return (widened * lax.rsqrt(lax.optimization_barrier(jnp.mean(widened * widened, axis=-1, keepdims=True)) + EPS) * gain).astype(jnp.bfloat16)

def rounded(value):
    return lax.optimization_barrier(value.astype(jnp.bfloat16)).astype(jnp.float32)

def reference(queries, keys, values, documents, query_gain, key_gain, out_weight, residual, norm_gain, up_weight, down_weight):
    positions = jnp.arange(PACKED_TOKENS, dtype=jnp.int32)
    rotated_query = rotate(head_norm(queries.astype(jnp.float32), query_gain), positions).astype(jnp.bfloat16)
    key_rot = rotate(head_norm(keys.astype(jnp.float32), key_gain), positions).astype(jnp.bfloat16)
    query_group_count = QUERY_HEADS // KEY_VALUE_HEADS
    key_wide = key_rot.astype(jnp.float32)
    value_wide = values.astype(jnp.float32)
    query_tiles = rotated_query.reshape(N_SP, TOKENS_PER_SHARD, KEY_VALUE_HEADS, query_group_count, HEAD_SIZE)
    doc_blocks = documents.reshape(N_SP, TOKENS_PER_SHARD)
    scale = HEAD_SIZE ** (-0.5)

    def attend(item):
        query_block, doc_block = item
        scores = jnp.einsum('qgrd,kgd->grqk', query_block.astype(jnp.float32), key_wide) * scale
        allowed = (doc_block[:, None] == documents[None, :])[None, None]
        scores = jnp.where(allowed, scores, -1e+30)
        peak = lax.optimization_barrier(jnp.max(scores, axis=-1, keepdims=True))
        probs = jnp.where(allowed, jnp.exp(scores - peak), 0.0)
        denom = lax.optimization_barrier(jnp.sum(probs, axis=-1))
        summed = jnp.einsum('grqk,kgd->qgrd', rounded(probs), value_wide)
        return (summed / jnp.transpose(denom, (2, 0, 1))[..., None]).astype(jnp.bfloat16)
    attn = lax.map(attend, (query_tiles, doc_blocks)).reshape(PACKED_TOKENS, QUERY_HEADS * HEAD_SIZE)
    span = QUERY_HEADS * HEAD_SIZE // N_TP
    branch = jnp.zeros((PACKED_TOKENS, D), jnp.float32)
    for index in range(N_TP):
        partial_term = jnp.dot(attn[:, index * span:(index + 1) * span], out_weight[index * span:(index + 1) * span], preferred_element_type=jnp.float32)
        branch = branch + rounded(partial_term)
    mid = (residual.astype(jnp.float32) + branch).astype(jnp.bfloat16)
    normed = channel_norm(mid, norm_gain)
    hidden_span = FF // N_TP
    mixer = jnp.zeros((PACKED_TOKENS, D), jnp.float32)
    for index in range(N_TP):
        raised = jnp.dot(normed, up_weight[:, index * hidden_span:(index + 1) * hidden_span], preferred_element_type=jnp.float32)
        hidden = jnp.square(jax.nn.relu(raised)).astype(jnp.bfloat16)
        partial_term = lax.dot_general(hidden, down_weight[:, index * hidden_span:(index + 1) * hidden_span], (((1,), (1,)), ((), ())), preferred_element_type=jnp.float32)
        mixer = mixer + rounded(partial_term)
    return (mid.astype(jnp.float32) + mixer).astype(jnp.bfloat16)
```

```python
import functools

import jax
import jax.numpy as jnp
import numpy as np
from jax import lax
from jax.experimental import pallas as pl
from jax.experimental.pallas import tpu as pltpu
from jax.sharding import PartitionSpec as P

QUERY_HEADS = 8
GRID = 64


EPS = 1e-06
THETA = 10000.0


def head_norm(block, gain):
    return block * lax.rsqrt(jnp.mean(block * block, axis=-1, keepdims=True) + EPS) * gain


def rotate(block, positions):
    head_width = block.shape[-1]
    pair_count = head_width // 4
    inverse = THETA ** (-jnp.arange(pair_count, dtype=jnp.float32) / pair_count)
    grid_row = (positions // GRID).astype(jnp.float32)[:, None] * inverse
    grid_col = (positions % GRID).astype(jnp.float32)[:, None] * inverse
    angles = jnp.concatenate([grid_row, grid_row, grid_col, grid_col], axis=-1)
    cosine = jnp.cos(angles)[:, None, :]
    sine_table = jnp.sin(angles)[:, None, :]
    turned = jnp.concatenate(
        [
            -block[..., pair_count : 2 * pair_count],
            block[..., 0:pair_count],
            -block[..., 3 * pair_count :],
            block[..., 2 * pair_count : 3 * pair_count],
        ],
        axis=-1,
    )
    return block * cosine + turned * sine_table


def channel_norm(rows_in, gain):
    widened = rows_in.astype(jnp.float32)
    return (
        widened * lax.rsqrt(jnp.mean(widened * widened, axis=-1, keepdims=True) + EPS) * gain
    ).astype(jnp.bfloat16)


def body(
    queries,
    keys,
    values,
    documents,
    query_gain,
    key_gain,
    out_weight,
    residual,
    norm_gain,
    up_weight,
    down_weight,
):
    tok_dev = queries.shape[0]
    heads_here = queries.shape[1]
    head_width = queries.shape[2]
    query_group_count = QUERY_HEADS // keys.shape[1]
    kv_index = lax.axis_index("tp") * heads_here // query_group_count
    positions = lax.axis_index("sp") * tok_dev + jnp.arange(tok_dev, dtype=jnp.int32)
    own_keys = lax.dynamic_index_in_dim(keys, kv_index, 1, keepdims=True)
    own_values = lax.dynamic_index_in_dim(values, kv_index, 1, keepdims=False)
    key_rot = rotate(head_norm(own_keys.astype(jnp.float32), key_gain), positions)[:, 0, :].astype(
        jnp.bfloat16
    )
    rotated_query = rotate(head_norm(queries.astype(jnp.float32), query_gain), positions).astype(
        jnp.bfloat16
    )
    scale = head_width ** (-0.5)
    first_doc = documents[0]
    last_doc = documents[tok_dev - 1]
    start_state = (
        jnp.full((tok_dev, heads_here), -1e30, jnp.float32),
        jnp.zeros((tok_dev, heads_here), jnp.float32),
        jnp.zeros((tok_dev, heads_here, head_width), jnp.float32),
    )
    piece_keys = lax.all_gather(key_rot, "sp", axis=0, tiled=True)
    piece_values = lax.all_gather(own_values, "sp", axis=0, tiled=True)
    piece_docs = lax.all_gather(documents, "sp", axis=0, tiled=True)

    def update(state):
        peak, denom, summed = state
        scores = (
            jnp.einsum("qhd,kd->qhk", rotated_query, piece_keys, preferred_element_type=jnp.float32)
            * scale
        )
        allowed = (documents[:, None] == piece_docs[None, :])[:, None, :]
        scores = jnp.where(allowed, scores, -1e30)
        new_peak = jnp.maximum(peak, jnp.max(scores, axis=-1))
        probs = jnp.where(allowed, jnp.exp(scores - new_peak[..., None]), 0.0)
        denom = jnp.sum(probs, axis=-1)
        summed = jnp.einsum(
            "qhk,kd->qhd",
            probs.astype(jnp.bfloat16),
            piece_values,
            preferred_element_type=jnp.float32,
        )
        return (new_peak, denom, summed)

    touches = jnp.logical_and(
        piece_docs[0] <= last_doc, piece_docs[piece_docs.shape[0] - 1] >= first_doc
    )
    peak, denom, summed = lax.cond(touches, update, lambda state: state, start_state)
    attn = (
        (summed / denom[..., None]).reshape(tok_dev, heads_here * head_width).astype(jnp.bfloat16)
    )
    share = tok_dev // lax.axis_size("tp")
    branch = lax.psum(
        jnp.dot(attn, out_weight, preferred_element_type=jnp.float32).astype(jnp.bfloat16), "tp"
    ).astype(jnp.float32)
    whole_rows = (residual.astype(jnp.float32) + branch).astype(jnp.bfloat16)
    normed = channel_norm(whole_rows, norm_gain)
    mid = lax.dynamic_slice_in_dim(whole_rows, lax.axis_index("tp") * share, share, 0)
    raised = jnp.dot(
        normed,
        lax.all_gather(up_weight, "sp", axis=0, tiled=True),
        preferred_element_type=jnp.float32,
    )
    hidden = jnp.square(jax.nn.relu(raised)).astype(jnp.bfloat16)
    terms = lax.dot_general(
        hidden,
        lax.all_gather(down_weight, "sp", axis=0, tiled=True),
        (((1,), (1,)), ((), ())),
        preferred_element_type=jnp.float32,
    )
    mixer = lax.psum_scatter(
        terms.astype(jnp.bfloat16), "tp", scatter_dimension=0, tiled=True
    ).astype(jnp.float32)
    return (mid.astype(jnp.float32) + mixer).astype(jnp.bfloat16)


MESH = pl.DeviceIdType.MESH
NT = (((1,), (1,)), ((), ()))
F32 = jnp.float32
BF16 = jnp.bfloat16


NEG = -1e30


def rope_tables(n_rows, width):
    quarter = width // 4
    steps = np.arange(quarter, dtype=np.float32) / np.float32(quarter)
    inverse = (np.float32(THETA) ** (-steps)).astype(np.float32)
    tables = []
    for f in (np.cos, np.sin):
        row, col = np.zeros((n_rows, width), np.float32), np.zeros((GRID, width), np.float32)
        for table, at in ((row, 0), (col, 2 * quarter)):
            angle = np.arange(table.shape[0], dtype=np.float32)[:, None] * inverse
            value = f(angle.astype(np.float64))
            table[:, at : at + quarter] = -value if f is np.sin else value
            table[:, at + quarter : at + 2 * quarter] = value
        tables += [row, col]
    return tables


def layer_kernel(
    q_hbm, k_hbm, v_hbm, doc_hbm, qg_hbm, kg_hbm, ow_hbm, res_hbm, ng_hbm, up_hbm, down_hbm,
    cr_hbm, cc_hbm, sr_hbm, sc_hbm, out_ref,
    q_raw, k_raw, v_raw, doc_v, qg, kg, ow, res, ng, cr, cc, sr, sc,
    q_rot, kv_all, dcol, bias, peak_s, den_s, acc_s, attn, wup, wdown, part, part_in, own_part,
    mid, tok, racc, hidden, outs, outs_in, sums, final_in,
    ld_s, own_s, kv_s, kv_r, w_s, w_r, p_s, p_r, t_s, t_r, o_s, o_r, f_s, f_r,
):
    rows, heads, width = q_raw.shape
    half = rows // 2
    piece = half // 2
    depth, cols = wup.shape[1], wup.shape[2]
    model = ow.shape[1]
    pair = 2 * depth
    sp, core = lax.axis_index("sp"), lax.axis_index("tp")
    x, y, z = sp % 2, (sp // 2) % 2, sp // 4
    zh = z // 2
    zmate = z + 1 - 2 * (z % 2)
    far = [2 - zh, 3 * (1 - zh)]
    zs = [z, zmate] + far
    zc = [2 * zh, 2 * zh + 1] + far

    def at(dx, dy, zz):
        return (zz * 2 + (y + dy) % 2) * 2 + (x + dx) % 2

    def rank(dx, zz):
        return zz % 2 * 2 + (x + dx) % 2

    sent = []

    def send(src, dst, ss, rs, spi, tpi):
        c = pltpu.make_async_remote_copy(
            src_ref=src, dst_ref=dst, send_sem=ss, recv_sem=rs,
            device_id=(spi, tpi), device_id_type=MESH,
        )
        c.start()
        sent.append(c)

    def arrive(dst, ss, rs):
        pltpu.make_async_remote_copy(
            src_ref=dst, dst_ref=dst, send_sem=ss, recv_sem=rs,
            device_id=(sp, 1 - core), device_id_type=MESH,
        ).wait_recv()

    loads = {}
    for i, (name, src, dst) in enumerate([
        ("k", k_hbm, k_raw), ("v", v_hbm, v_raw), ("doc", doc_hbm, doc_v), ("kg", kg_hbm, kg),
        ("cr", cr_hbm, cr), ("cc", cc_hbm, cc), ("sr", sr_hbm, sr), ("sc", sc_hbm, sc),
        ("q", q_hbm, q_raw), ("qg", qg_hbm, qg), ("ow", ow_hbm, ow), ("res", res_hbm, res),
        ("ng", ng_hbm, ng),
    ]):
        loads[name] = pltpu.make_async_copy(src, dst, ld_s.at[i])
        loads[name].start()
    weights = ((up_hbm, wup), (down_hbm, wdown))

    def columns(w, dx, zz):
        return weights[w][0].at[:, pl.ds(pl.multiple_of(rank(dx, zz) * cols, 128), cols)]

    own = []
    for w in (0, 1):
        own.append(pltpu.make_async_copy(columns(w, 0, z), weights[w][1].at[sp], own_s.at[w]))
        own[w].start()

    barrier = pltpu.get_barrier_semaphore()
    peers = [(at(dx, 0, zs[k]), core) for dx in (0, 1) for k in range(4) if dx or k]
    peers += [(at(0, 1, z), core), (sp, 1 - core)]
    for p in peers:
        pl.semaphore_signal(barrier, inc=1, device_id=p, device_id_type=MESH)

    def wait_loads(*names):
        for name in names:
            loads[name].wait()

    wait_loads("k", "v", "doc", "kg", "cr", "cc", "sr", "sc")
    grid_rows = rows // GRID

    def table(row, col):
        lines = row[pl.ds(sp * grid_rows, grid_rows)]
        return (lines[:, None, :] + col[...][None]).reshape(rows, width)

    cosine, sine = table(cr, cc), table(sr, sc)
    first = lax.broadcasted_iota(jnp.int32, (rows, width), 1) % (width // 2) < width // 4

    def norm_rope(v, gain):
        v = v * lax.rsqrt(jnp.mean(v * v, axis=-1, keepdims=True) + EPS) * gain[...]
        turned = jnp.where(
            first, pltpu.roll(v, width - width // 4, 1), pltpu.roll(v, width // 4, 1)
        )
        return (v * cosine + turned * sine).astype(BF16)

    def own_head(ref):
        both = ref[...].astype(F32)
        return jnp.where(core == 0, both[:, 0, :], both[:, 1, :])

    kv_all[sp, 0:rows] = norm_rope(own_head(k_raw), kg)
    kv_all[sp, rows : 2 * rows] = own_head(v_raw).astype(BF16)
    docs = doc_v[...].astype(F32)
    lines = [docs[:, i * width : (i + 1) * width] for i in range(rows // width)]
    pad = kv_all.shape[1] - 2 * rows - len(lines)
    lines.append(jnp.zeros((pad, width), F32))
    kv_all[sp, 2 * rows :] = jnp.concatenate(lines, axis=0).astype(BF16)

    pl.semaphore_wait(barrier, len(peers))

    def send_kv(i, slot, spi):
        send(kv_all.at[slot], kv_all.at[slot], kv_s.at[i], kv_r.at[slot], spi, core)

    def wait_kv(slot):
        arrive(kv_all.at[slot], kv_s.at[0], kv_r.at[slot])

    def send_weight(w, dx, k):
        target = at(dx, 0, zs[k])
        send(
            columns(w, dx, zs[k]), weights[w][1].at[sp],
            w_s.at[w, dx * 4 + k], w_r.at[w, sp], target, core,
        )

    def wait_weight(w, dx, dy, zz):
        i = at(dx, dy, zz)
        arrive(weights[w][1].at[i], w_s.at[w, 0], w_r.at[w, i])

    def forward_weight(w, dx, k):
        i = at(dx, 0, zs[k])
        dst = weights[w][1]
        if dx or k:
            wait_weight(w, dx, 0, zs[k])
            src = dst.at[i]
        else:
            src = columns(w, 0, z)
        send(src, dst.at[i], w_s.at[w, 8 + dx * 4 + k], w_r.at[w, i], at(0, 1, z), core)

    for k in (1, 2, 3):
        send_kv(k, sp, at(0, 0, zs[k]))
    send_kv(0, sp, at(1, 0, z))
    send_kv(4, sp, at(0, 1, z))
    for k in (1, 2, 3):
        send_weight(0, 0, k)

    wait_loads("q", "qg")
    wide = q_raw[...].astype(F32)
    for h in range(heads):
        q_rot[h] = norm_rope(wide[:, h, :], qg)
    dcol[...] = jnp.broadcast_to(docs, (width, rows)).T

    for k in (1, 2, 3):
        i = at(0, 0, zs[k])
        wait_kv(i)
        send_kv(4 + k, i, at(1, 0, z))
        send_kv(8 + k, i, at(0, 1, z))

    for h in range(heads):
        lines = pl.ds(h * rows, rows)
        peak_s[lines] = jnp.full((rows, width), NEG, F32)
        den_s[lines] = jnp.zeros((rows, width), F32)
        acc_s[lines] = jnp.zeros((rows, width), F32)
    scale = float(width ** (-0.5) * np.log2(np.e))
    tiles = rows // width

    def attend(slots):
        for b, i in enumerate(slots):
            theirs = kv_all[i, 2 * rows :].astype(F32)
            for t in range(tiles):
                bias[:, (b * tiles + t) * width : (b * tiles + t + 1) * width] = jnp.where(
                    dcol[...] == theirs[t : t + 1], 0.0, NEG
                )
        for h in range(heads):
            lines = pl.ds(h * rows, rows)
            scores = []
            for b, i in enumerate(slots):
                s = lax.dot_general(
                    q_rot[h], kv_all[i, 0:rows], NT, preferred_element_type=F32
                )
                scores.append(s * scale + bias[:, b * rows : (b + 1) * rows])
            top = functools.reduce(
                jnp.maximum,
                [s[:, t * width : (t + 1) * width] for s in scores for t in range(tiles)],
            )
            peak = peak_s[lines]
            new_peak = jnp.maximum(peak, jnp.max(top, axis=-1, keepdims=True))
            peak_s[lines] = new_peak
            decay = jnp.exp2(peak - new_peak)
            spread = jnp.concatenate([new_peak] * tiles, axis=1)
            probs = [jnp.exp2(s - spread) for s in scores]
            den_s[lines] = den_s[lines] * decay + functools.reduce(
                jnp.add,
                [p[:, t * width : (t + 1) * width] for p in probs for t in range(tiles)],
            )
            acc_s[lines] = acc_s[lines] * decay + functools.reduce(
                jnp.add,
                [
                    jnp.dot(p.astype(BF16), kv_all[i, rows : 2 * rows], preferred_element_type=F32)
                    for i, p in zip(slots, probs)
                ],
            )

    def column(dx, dy):
        return [at(dx, dy, zz) for zz in zs]

    attend(column(0, 0))
    for k in (0, 1):
        i = at(1, 0, zs[k])
        wait_kv(i)
        send_kv(12 + k, i, at(0, 1, z))
    for k in (0, 1):
        wait_kv(at(0, 1, zs[k]))
    for k in (2, 3):
        i = at(0, 1, zs[k])
        wait_kv(i)
        send_kv(12 + k, i, at(1, 0, z))
    for k in (2, 3):
        wait_kv(at(1, 0, zs[k]))
    for k in (0, 1, 2, 3):
        send_weight(0, 1, k)
    forward_weight(0, 0, 0)
    attend(column(1, 0))
    attend(column(0, 1))
    forward_weight(0, 0, 1)
    for k in range(4):
        wait_kv(at(1, 1, zs[k]))
    attend(column(1, 1))
    forward_weight(0, 1, 0)
    for h in range(heads):
        lines = pl.ds(h * rows, rows)
        denom = jnp.sum(den_s[lines], axis=-1, keepdims=True)
        attn[:, h * width : (h + 1) * width] = (acc_s[lines] / denom).astype(BF16)

    tile = 256
    wait_loads("ow", "res", "ng")

    def project(owner, p, dst):
        mine = pl.ds(pl.multiple_of(owner * half + p * piece, piece), piece)

        @pl.loop(0, model // (2 * tile))
        def _(t):
            lanes = pl.ds(pl.multiple_of(t * 2 * tile, 2 * tile), 2 * tile)
            dst[p, :, lanes] = jnp.dot(
                attn[mine], ow[:, lanes], preferred_element_type=F32
            ).astype(BF16)

    for p in (0, 1):
        project(1 - core, p, part)
        send(part.at[p], part_in.at[p], p_s.at[p], p_r.at[p], sp, 1 - core)
    for p in (0, 1):
        project(core, p, own_part)
    group = 32
    xm, zm = at(1, 0, z), at(0, 0, zmate)
    n_tok = [0]

    def send_tok(src, dst, p, spi, tpi):
        i = n_tok[0]
        n_tok[0] += 1
        rc, c = dst
        send(tok.at[src[0], src[1], p], tok.at[rc, c, p], t_s.at[i], t_r.at[rc, c, p], spi, tpi)

    def wait_tok(rc, c, p):
        arrive(tok.at[rc, c, p], t_s.at[0], t_r.at[rc, c, p])

    for p in (0, 1):
        arrive(part_in.at[p], p_s.at[p], p_r.at[p])

        @pl.loop(0, piece // group)
        def _(t):
            rws = pl.ds(pl.multiple_of(t * group, group), group)
            branch = own_part[p, rws].astype(F32) + part_in[p, rws].astype(F32)
            rres = pl.ds(pl.multiple_of(core * half + p * piece + t * group, group), group)
            m = (res[rres].astype(F32) + branch).astype(BF16)
            mid[pl.ds(pl.multiple_of(p * piece + t * group, group), group)] = m
            full = m.astype(F32)
            inv = lax.rsqrt(jnp.mean(full * full, axis=-1, keepdims=True) + EPS)
            tok[0, 0, p, rws] = (full * inv * ng[...]).astype(BF16)

        if p == 0:
            send_tok((0, 0), (1, 0), 0, xm, core)
            send_tok((0, 0), (0, 1), 0, sp, 1 - core)
        else:
            send_tok((0, 0), (2, 0), 1, zm, core)
            send_tok((0, 0), (0, 1), 1, sp, 1 - core)
    send_tok((0, 0), (2, 0), 0, zm, core)
    send_tok((0, 0), (1, 0), 1, xm, core)
    forward_weight(0, 1, 1)
    wait_tok(1, 0, 0)
    send_tok((1, 0), (3, 0), 0, zm, core)
    send_tok((1, 0), (1, 1), 0, sp, 1 - core)
    wait_tok(2, 0, 1)
    send_tok((2, 0), (3, 0), 1, xm, core)
    send_tok((2, 0), (2, 1), 1, sp, 1 - core)
    for k in (1, 2, 3):
        send_weight(1, 0, k)
    for k in (0, 1, 2, 3):
        send_weight(1, 1, k)
    for k in (2, 3):
        for dx in (0, 1):
            forward_weight(0, dx, k)
    forward_weight(1, 0, 0)
    own[0].wait()
    wait_tok(1, 0, 1)
    send_tok((1, 0), (1, 1), 1, sp, 1 - core)
    wait_tok(2, 0, 0)
    send_tok((2, 0), (2, 1), 0, sp, 1 - core)
    for p in (0, 1):
        wait_tok(3, 0, p)
        send_tok((3, 0), (3, 1), p, sp, 1 - core)

    def raise_part(rc, dy, last):
        @pl.loop(0, cols // tile)
        def _(t):
            lanes = pl.ds(pl.multiple_of(t * tile, tile), tile)
            total = None
            for zz in range(4):
                block = (zz * 2 + (y + dy) % 2) * 2
                feats = pl.ds(pl.multiple_of(block * depth, pair), pair)
                tokens = tok[rc, :, :, :, feats].reshape(rows, pair)
                w = wup[pl.ds(block, 2), :, lanes].reshape(pair, tile)
                term = jnp.dot(tokens, w, preferred_element_type=F32)
                total = term if total is None else total + term
            if last:
                total = racc[rc, :, lanes] + total
                hidden[rc, :, lanes] = jnp.square(jnp.maximum(total, 0.0)).astype(BF16)
            else:
                racc[rc, :, lanes] = total

    for rc in range(4):
        for p in (0, 1):
            wait_tok(rc, 1, p)
        raise_part(rc, 0, False)
    for k in range(4):
        for dx in (0, 1):
            wait_weight(0, dx, 1, zs[k])
    for rc in range(4):
        raise_part(rc, 1, True)

    own[1].wait()

    def lower(j, dy, zz):
        block = (zz * 2 + (y + dy) % 2) * 2
        w = wdown[pl.ds(block, 2)].reshape(pair, cols)
        for rc in range(4):
            o = lax.dot_general(hidden[rc], w, NT, preferred_element_type=F32).astype(BF16)
            outs[j, 0, rc] = o[:half]
            outs[j, 1, rc] = o[half:]
        send(outs.at[j, 1], outs_in.at[j], o_s.at[j], o_r.at[j], sp, 1 - core)

    mates = (None, xm, zm, at(1, 0, zmate))

    def combine(j):
        arrive(outs_in.at[j], o_s.at[j], o_r.at[j])
        for rc in (3, 1, 2):
            sums[j, rc - 1] = (
                outs[j, 0, rc].astype(F32) + outs_in[j, rc].astype(F32)
            ).astype(BF16)
            send(
                sums.at[j, rc - 1], final_in.at[j, rc - 1],
                f_s.at[j, rc - 1], f_r.at[j, rc - 1], mates[rc], core,
            )

    def finish(j, dy, zz):
        block = (zz * 2 + (y + dy) % 2) * 2
        total = outs[j, 0, 0].astype(F32) + outs_in[j, 0].astype(F32)
        for rc in (1, 2, 3):
            arrive(final_in.at[j, rc - 1], f_s.at[j, rc - 1], f_r.at[j, rc - 1])
            total += final_in[j, rc - 1].astype(F32)
        lanes = pl.ds(pl.multiple_of(block * depth, pair), pair)
        out_ref[:, lanes] = (mid[:, lanes].astype(F32) + total).astype(BF16)

    order = [(0, 0), (0, 1), (1, 0), (1, 1), (0, 2), (1, 2), (0, 3), (1, 3)]
    for j, (dy, k) in enumerate(order):
        if dy == 0:
            if k == 0:
                for dx, kk in ((1, 0), (0, 1), (1, 1)):
                    forward_weight(1, dx, kk)
            elif k > 1:
                for dx in (0, 1):
                    forward_weight(1, dx, k)
        else:
            for dx in (0, 1):
                wait_weight(1, dx, 1, zc[k])
        lower(j, dy, zc[k])
        combine(j)
        if j >= 3:
            finish(j - 3, order[j - 3][0], zc[order[j - 3][1]])
    for j in range(5, 8):
        finish(j, order[j][0], zc[order[j][1]])

    for c in sent:
        c.wait_send()


def fused_body(
    queries, keys, values, documents, query_gain, key_gain, out_weight, residual, norm_gain,
    up_weight, down_weight,
):
    rows, heads, width = queries.shape
    n_sp = lax.axis_size("sp")
    model = residual.shape[1]
    depth, cols = up_weight.shape[0], up_weight.shape[1] // 4
    half = rows // 2
    piece = half // 2
    pair = 2 * depth
    chunks = model // pair
    dma = pltpu.SemaphoreType.DMA
    vmem = pltpu.VMEM
    tables = rope_tables(n_sp * rows // GRID, width)
    operands = (
        queries, keys, values, documents[None, :], query_gain[None, :], key_gain[None, :],
        out_weight, residual, norm_gain[None, :], up_weight, down_weight, *tables,
    )
    loaded = [a for i, a in enumerate(operands) if i not in (9, 10)]
    return pl.pallas_call(
        layer_kernel,
        out_shape=jax.ShapeDtypeStruct((half, model), BF16),
        in_specs=[pl.BlockSpec(memory_space=pl.ANY)] * len(operands),
        out_specs=pl.BlockSpec(memory_space=pltpu.VMEM),
        scratch_shapes=[vmem(a.shape, a.dtype) for a in loaded] + [
            vmem((heads, rows, width), BF16),
            vmem((n_sp, 2 * rows + 16, width), BF16),
            vmem((rows, width), F32),
            vmem((rows, 4 * rows), F32),
            vmem((heads * rows, width), F32),
            vmem((heads * rows, width), F32),
            vmem((heads * rows, width), F32),
            vmem((rows, heads * width), BF16),
            vmem((n_sp, depth, cols), BF16),
            vmem((n_sp, depth, cols), BF16),
            vmem((2, piece, model), BF16),
            vmem((2, piece, model), BF16),
            vmem((2, piece, model), BF16),
            vmem((half, model), BF16),
            vmem((4, 2, 2, piece, model), BF16),
            vmem((4, rows, cols), F32),
            vmem((4, rows, cols), BF16),
            vmem((chunks, 2, 4, half, pair), BF16),
            vmem((chunks, 4, half, pair), BF16),
            vmem((chunks, 3, half, pair), BF16),
            vmem((chunks, 3, half, pair), BF16),
            dma((13,)), dma((2,)), dma((16,)), dma((n_sp,)), dma((2, 16)), dma((2, n_sp)),
            dma((2,)), dma((2,)), dma((16,)), dma((4, 2, 2)), dma((chunks,)), dma((chunks,)),
            dma((chunks, 3)), dma((chunks, 3)),
        ],
        compiler_params=pltpu.CompilerParams(
            collective_id=0, has_side_effects=True, vmem_limit_bytes=60 * 1024 * 1024
        ),
    )(*operands)


def solution(mesh):
    in_specs = (
        P("sp", "tp", None),
        P("sp", None, None),
        P("sp", None, None),
        P("sp"),
        P(),
        P(),
        P("tp", None),
        P("sp", None),
        P(),
        P("sp", "tp"),
        P("sp", "tp"),
    )
    out_specs = P(("sp", "tp"), None)
    fused = mesh.shape["tp"] == 2 and mesh.shape["sp"] == 16
    return jax.shard_map(fused_body if fused else body, mesh=mesh, in_specs=in_specs, out_specs=out_specs, check_vma=False)
```

```python
import functools

import jax
import jax.numpy as jnp
import numpy as np
from jax import lax
from jax.experimental import pallas as pl
from jax.experimental.pallas import tpu as pltpu
from jax.sharding import PartitionSpec as P

QUERY_HEADS = 8
GRID = 64


EPS = 1e-06
THETA = 10000.0


def head_norm(block, gain):
    return block * lax.rsqrt(jnp.mean(block * block, axis=-1, keepdims=True) + EPS) * gain


def rotate(block, positions):
    head_width = block.shape[-1]
    pair_count = head_width // 4
    inverse = THETA ** (-jnp.arange(pair_count, dtype=jnp.float32) / pair_count)
    grid_row = (positions // GRID).astype(jnp.float32)[:, None] * inverse
    grid_col = (positions % GRID).astype(jnp.float32)[:, None] * inverse
    angles = jnp.concatenate([grid_row, grid_row, grid_col, grid_col], axis=-1)
    cosine = jnp.cos(angles)[:, None, :]
    sine_table = jnp.sin(angles)[:, None, :]
    turned = jnp.concatenate(
        [
            -block[..., pair_count : 2 * pair_count],
            block[..., 0:pair_count],
            -block[..., 3 * pair_count :],
            block[..., 2 * pair_count : 3 * pair_count],
        ],
        axis=-1,
    )
    return block * cosine + turned * sine_table


def channel_norm(rows_in, gain):
    widened = rows_in.astype(jnp.float32)
    return (
        widened * lax.rsqrt(jnp.mean(widened * widened, axis=-1, keepdims=True) + EPS) * gain
    ).astype(jnp.bfloat16)


def body(
    queries,
    keys,
    values,
    documents,
    query_gain,
    key_gain,
    out_weight,
    residual,
    norm_gain,
    up_weight,
    down_weight,
):
    tok_dev = queries.shape[0]
    heads_here = queries.shape[1]
    head_width = queries.shape[2]
    query_group_count = QUERY_HEADS // keys.shape[1]
    kv_index = lax.axis_index("tp") * heads_here // query_group_count
    positions = lax.axis_index("sp") * tok_dev + jnp.arange(tok_dev, dtype=jnp.int32)
    own_keys = lax.dynamic_index_in_dim(keys, kv_index, 1, keepdims=True)
    own_values = lax.dynamic_index_in_dim(values, kv_index, 1, keepdims=False)
    key_rot = rotate(head_norm(own_keys.astype(jnp.float32), key_gain), positions)[:, 0, :].astype(
        jnp.bfloat16
    )
    rotated_query = rotate(head_norm(queries.astype(jnp.float32), query_gain), positions).astype(
        jnp.bfloat16
    )
    scale = head_width ** (-0.5)
    first_doc = documents[0]
    last_doc = documents[tok_dev - 1]
    start_state = (
        jnp.full((tok_dev, heads_here), -1e30, jnp.float32),
        jnp.zeros((tok_dev, heads_here), jnp.float32),
        jnp.zeros((tok_dev, heads_here, head_width), jnp.float32),
    )
    piece_keys = lax.all_gather(key_rot, "sp", axis=0, tiled=True)
    piece_values = lax.all_gather(own_values, "sp", axis=0, tiled=True)
    piece_docs = lax.all_gather(documents, "sp", axis=0, tiled=True)

    def update(state):
        peak, denom, summed = state
        scores = (
            jnp.einsum("qhd,kd->qhk", rotated_query, piece_keys, preferred_element_type=jnp.float32)
            * scale
        )
        allowed = (documents[:, None] == piece_docs[None, :])[:, None, :]
        scores = jnp.where(allowed, scores, -1e30)
        new_peak = jnp.maximum(peak, jnp.max(scores, axis=-1))
        probs = jnp.where(allowed, jnp.exp(scores - new_peak[..., None]), 0.0)
        denom = jnp.sum(probs, axis=-1)
        summed = jnp.einsum(
            "qhk,kd->qhd",
            probs.astype(jnp.bfloat16),
            piece_values,
            preferred_element_type=jnp.float32,
        )
        return (new_peak, denom, summed)

    touches = jnp.logical_and(
        piece_docs[0] <= last_doc, piece_docs[piece_docs.shape[0] - 1] >= first_doc
    )
    peak, denom, summed = lax.cond(touches, update, lambda state: state, start_state)
    attn = (
        (summed / denom[..., None]).reshape(tok_dev, heads_here * head_width).astype(jnp.bfloat16)
    )
    share = tok_dev // lax.axis_size("tp")
    branch = lax.psum(
        jnp.dot(attn, out_weight, preferred_element_type=jnp.float32).astype(jnp.bfloat16), "tp"
    ).astype(jnp.float32)
    whole_rows = (residual.astype(jnp.float32) + branch).astype(jnp.bfloat16)
    normed = channel_norm(whole_rows, norm_gain)
    mid = lax.dynamic_slice_in_dim(whole_rows, lax.axis_index("tp") * share, share, 0)
    raised = jnp.dot(
        normed,
        lax.all_gather(up_weight, "sp", axis=0, tiled=True),
        preferred_element_type=jnp.float32,
    )
    hidden = jnp.square(jax.nn.relu(raised)).astype(jnp.bfloat16)
    terms = lax.dot_general(
        hidden,
        lax.all_gather(down_weight, "sp", axis=0, tiled=True),
        (((1,), (1,)), ((), ())),
        preferred_element_type=jnp.float32,
    )
    mixer = lax.psum_scatter(
        terms.astype(jnp.bfloat16), "tp", scatter_dimension=0, tiled=True
    ).astype(jnp.float32)
    return (mid.astype(jnp.float32) + mixer).astype(jnp.bfloat16)


MESH = pl.DeviceIdType.MESH
NT = (((1,), (1,)), ((), ()))
F32 = jnp.float32
BF16 = jnp.bfloat16


NEG = -1e30
CHUNKS = ((0, 0), (0, 1), (1, 0), (0, 2), (1, 1), (0, 3), (1, 2), (1, 3))
STRAIGHT = 0
SCHEDULE = (
    "K1", "K2", "K3", "n001", "n002", "n003", "A0", "R0", "R1", "A1",
    "A2", "y000", "n010", "n011", "A3", "y001", "P0", "y010", "M0", "x0",
    "M1", "z1", "z0", "x1", "n012", "n013", "n110", "n101", "n111", "m102",
    "m112", "m103", "m113", "y011", "r10", "r21", "e102", "e112", "e103", "e113",
    "y002", "y003", "y100", "y012", "y013", "U0", "r11", "r20", "U1", "U2",
    "y110", "y101", "y111", "r30", "r31", "U3", "V0", "L0", "C0", "L1",
    "C1", "y102", "y112", "L2", "C2", "Z0", "L3", "C3", "Z1", "y103",
    "y113", "L4", "C4", "Z2", "F0", "L5", "C5", "Z3", "F1", "L6",
    "C6", "Z4", "F2", "L7", "C7", "Z5", "Z6", "Z7", "F3", "F4",
    "F5", "F6", "F7",
)


def rope_tables(n_rows, width):
    quarter = width // 4
    steps = np.arange(quarter, dtype=np.float32) / np.float32(quarter)
    inverse = (np.float32(THETA) ** (-steps)).astype(np.float32)
    tables = []
    for f in (np.cos, np.sin):
        row, col = np.zeros((n_rows, width), np.float32), np.zeros((GRID, width), np.float32)
        for table, at in ((row, 0), (col, 2 * quarter)):
            angle = np.arange(table.shape[0], dtype=np.float32)[:, None] * inverse
            value = f(angle.astype(np.float64))
            table[:, at : at + quarter] = -value if f is np.sin else value
            table[:, at + quarter : at + 2 * quarter] = value
        tables += [row, col]
    return tables


def layer_kernel(
    q_hbm, k_hbm, v_hbm, doc_hbm, qg_hbm, kg_hbm, ow_hbm, res_hbm, ng_hbm, up_hbm, down_hbm,
    cr_hbm, cc_hbm, sr_hbm, sc_hbm, out_ref,
    q_raw, k_raw, v_raw, doc_v, qg, kg, ow, res, ng, cr, cc, sr, sc,
    q_rot, kv_all, dcol, bias, peak_s, den_s, acc_s, attn, wup, wdown, part, part_in, own_part,
    mid, tok, racc, hidden, outs, outs_in, sums, final_in,
    ld_s, own_s, kv_s, kv_r, w_s, w_r, p_s, p_r, t_s, t_r, o_s, o_r, f_s, f_r,
):
    rows, heads, width = q_raw.shape
    half = rows // 2
    piece = half // 2
    depth, cols = wup.shape[1], wup.shape[2]
    model = ow.shape[1]
    pair = 2 * depth
    sp, core = lax.axis_index("sp"), lax.axis_index("tp")
    x, y, z = sp % 2, (sp // 2) % 2, sp // 4
    zh = z // 2
    zmate = z + 1 - 2 * (z % 2)
    far = [2 - zh, 3 * (1 - zh)]
    zs = [z, zmate] + far
    zc = [2 * zh, 2 * zh + 1] + far

    def at(dx, dy, zz):
        return (zz * 2 + (y + dy) % 2) * 2 + (x + dx) % 2

    def rank(dx, zz):
        return zz % 2 * 2 + (x + dx) % 2

    sent = []

    inner = (z == 1) | (z == 2)
    n_sp = kv_all.shape[0]
    reach = n_sp // 2 + 1
    low = n_sp // 4 - 1
    lone = (sp == low) | (sp == low + reach)
    across = jnp.where(sp == low, low + reach, low)
    sometimes = []

    def send(src, dst, ss, rs, spi, tpi, start=True, cond=None):
        c = pltpu.make_async_remote_copy(
            src_ref=src, dst_ref=dst, send_sem=ss, recv_sem=rs,
            device_id=(spi, tpi), device_id_type=MESH,
        )
        if cond is not None:
            pl.when(cond)(c.start)
            sometimes.append((cond, c))
            return
        if start:
            c.start()
        sent.append(c)

    def arrive(dst, ss, rs):
        pltpu.make_async_remote_copy(
            src_ref=dst, dst_ref=dst, send_sem=ss, recv_sem=rs,
            device_id=(sp, 1 - core), device_id_type=MESH,
        ).wait_recv()

    loads = {}
    for i, (name, src, dst) in enumerate([
        ("k", k_hbm, k_raw), ("v", v_hbm, v_raw), ("doc", doc_hbm, doc_v), ("kg", kg_hbm, kg),
        ("cr", cr_hbm, cr), ("cc", cc_hbm, cc), ("sr", sr_hbm, sr), ("sc", sc_hbm, sc),
        ("q", q_hbm, q_raw), ("qg", qg_hbm, qg), ("ow", ow_hbm, ow), ("res", res_hbm, res),
        ("ng", ng_hbm, ng),
    ]):
        loads[name] = pltpu.make_async_copy(src, dst, ld_s.at[i])
        loads[name].start()
    weights = ((up_hbm, wup), (down_hbm, wdown))

    def columns(w, dx, zz):
        return weights[w][0].at[:, pl.ds(pl.multiple_of(rank(dx, zz) * cols, 128), cols)]

    own = []
    for w in (0, 1):
        own.append(pltpu.make_async_copy(columns(w, 0, z), weights[w][1].at[sp], own_s.at[w]))
        own[w].start()

    barrier = pltpu.get_barrier_semaphore()
    peers = [(at(0, 0, zz), core) for zz in zs[1:]]
    peers += [(at(1, 0, z), core), (at(1, 0, zmate), core), (at(0, 1, z), core), (sp, 1 - core)]
    peers += [(at(1, 1, 3 - z), core)]
    for p in peers:
        pl.semaphore_signal(barrier, inc=1, device_id=p, device_id_type=MESH)


    def wait_loads(*names):
        for name in names:
            loads[name].wait()

    wait_loads("k", "v", "doc", "kg", "cr", "cc", "sr", "sc")
    grid_rows = rows // GRID

    def table(row, col):
        lines = row[pl.ds(sp * grid_rows, grid_rows)]
        return (lines[:, None, :] + col[...][None]).reshape(rows, width)

    cosine, sine = table(cr, cc), table(sr, sc)
    first = lax.broadcasted_iota(jnp.int32, (rows, width), 1) % (width // 2) < width // 4

    def norm_rope(v, gain):
        v = v * lax.rsqrt(jnp.mean(v * v, axis=-1, keepdims=True) + EPS) * gain[...]
        turned = jnp.where(
            first, pltpu.roll(v, width - width // 4, 1), pltpu.roll(v, width // 4, 1)
        )
        return (v * cosine + turned * sine).astype(BF16)

    def own_head(ref):
        both = ref[...].astype(F32)
        return jnp.where(core == 0, both[:, 0, :], both[:, 1, :])

    kv_all[sp, 0:rows] = norm_rope(own_head(k_raw), kg)
    kv_all[sp, rows : 2 * rows] = own_head(v_raw).astype(BF16)
    docs = doc_v[...].astype(F32)
    lines = [docs[:, i * width : (i + 1) * width] for i in range(rows // width)]
    pad = kv_all.shape[1] - 2 * rows - len(lines)
    lines.append(jnp.zeros((pad, width), F32))
    kv_all[sp, 2 * rows :] = jnp.concatenate(lines, axis=0).astype(BF16)

    for dx, dy in ((0, 0), (1, 0), (0, 1), (1, 1)):
        empty = at(dx, dy, zs[3])

        @pl.when(jnp.logical_not(inner | (lone & (empty == across))))
        def _():
            kv_all[empty] = jnp.full(kv_all.shape[1:], -1.0, BF16)

    pl.semaphore_wait(barrier, len(peers))


    def send_kv(i, slot, spi, cond=None):
        send(
            kv_all.at[slot], kv_all.at[slot], kv_s.at[i], kv_r.at[slot], spi, core, cond=cond
        )

    def only(k):
        return inner if k == 3 else None

    def wait_kv(slot, cond=None):
        if cond is not None:
            pl.when(cond)(lambda: wait_kv(slot))
            return
        arrive(kv_all.at[slot], kv_s.at[0], kv_r.at[slot])

    def send_weight(w, dx, k, start=True):
        send(
            columns(w, dx, zs[k]), weights[w][1].at[sp],
            w_s.at[w, dx * 4 + k], w_r.at[w, sp], at(dx, 0, zs[k]), core, start,
        )

    def send_weight_if(cond, w, dx, k):
        count = len(sent)
        pl.when(cond)(lambda: send_weight(w, dx, k))
        del sent[count:]

    def wait_weight(w, dx, dy, zz):
        i = at(dx, dy, zz)
        arrive(weights[w][1].at[i], w_s.at[w, 0], w_r.at[w, i])

    def pass_weight(w, dx, k, across):
        i = at(dx, 0, zs[k])
        dst = weights[w][1]
        src = dst.at[i] if dx or k else columns(w, 0, z)
        send(
            src, dst.at[i], w_s.at[w, (16 if across else 8) + dx * 4 + k], w_r.at[w, i],
            at(0, 0, (z + 2) % 4) if across else at(0, 1, z), core,
        )

    for k in (1, 2, 3):
        send_kv(k, sp, at(0, 0, zs[k]), only(k))
    send_kv(0, sp, at(1, 0, z))
    send_kv(4, sp, at(0, 1, z))
    send_kv(16, sp, across, lone)

    wait_loads("q", "qg")
    wide = q_raw[...].astype(F32)
    for h in range(heads):
        q_rot[h] = norm_rope(wide[:, h, :], qg)
    dcol[...] = jnp.broadcast_to(docs, (width, rows)).T

    for h in range(heads):
        lines = pl.ds(h * rows, rows)
        peak_s[lines] = jnp.full((rows, width), NEG, F32)
        den_s[lines] = jnp.zeros((rows, width), F32)
        acc_s[lines] = jnp.zeros((rows, width), F32)
    scale = float(width ** (-0.5) * np.log2(np.e))
    tiles = rows // width

    def attend(slots):
        for b, i in enumerate(slots):
            theirs = kv_all[i, 2 * rows :].astype(F32)
            for t in range(tiles):
                bias[:, (b * tiles + t) * width : (b * tiles + t + 1) * width] = jnp.where(
                    dcol[...] == theirs[t : t + 1], 0.0, NEG
                )
        for h in range(heads):
            lines = pl.ds(h * rows, rows)
            scores = []
            for b, i in enumerate(slots):
                s = lax.dot_general(
                    q_rot[h], kv_all[i, 0:rows], NT, preferred_element_type=F32
                )
                scores.append(s * scale + bias[:, b * rows : (b + 1) * rows])
            top = functools.reduce(
                jnp.maximum,
                [s[:, t * width : (t + 1) * width] for s in scores for t in range(tiles)],
            )
            peak = peak_s[lines]
            new_peak = jnp.maximum(peak, jnp.max(top, axis=-1, keepdims=True))
            peak_s[lines] = new_peak
            decay = jnp.exp2(peak - new_peak)
            spread = jnp.concatenate([new_peak] * tiles, axis=1)
            probs = [jnp.exp2(s - spread) for s in scores]
            den_s[lines] = den_s[lines] * decay + functools.reduce(
                jnp.add,
                [p[:, t * width : (t + 1) * width] for p in probs for t in range(tiles)],
            )
            acc_s[lines] = acc_s[lines] * decay + functools.reduce(
                jnp.add,
                [
                    jnp.dot(p.astype(BF16), kv_all[i, rows : 2 * rows], preferred_element_type=F32)
                    for i, p in zip(slots, probs)
                ],
            )

    def column(dx, dy):
        return [at(dx, dy, zz) for zz in zs]

    def relay_z(k):
        i = at(0, 0, zs[k])
        wait_kv(i, only(k))
        send_kv(4 + k, i, at(1, 0, z), only(k))
        send_kv(8 + k, i, at(0, 1, z), only(k))

    def relay_y():
        for k in (0, 1):
            i = at(1, 0, zs[k])
            wait_kv(i)
            send_kv(12 + k, i, at(0, 1, z))

    def relay_x():
        for k in (2, 3):
            i = at(0, 1, zs[k])
            wait_kv(i, only(k))
            send_kv(12 + k, i, at(1, 0, z), only(k))

    def attend_column(dx, dy, ks):
        for k in ks:
            wait_kv(at(dx, dy, zs[k]), only(k))
        if dx and dy:
            wait_kv(across, lone)
        attend(column(dx, dy))

    def attention_out():
        for h in range(heads):
            lines = pl.ds(h * rows, rows)
            denom = jnp.sum(den_s[lines], axis=-1, keepdims=True)
            attn[:, h * width : (h + 1) * width] = (acc_s[lines] / denom).astype(BF16)

    tile = 256

    def project(owner, dst):
        mine = pl.ds(pl.multiple_of(owner * half, half), half)
        wide = 4 * tile

        @pl.loop(0, model // wide)
        def _(t):
            lanes = pl.ds(pl.multiple_of(t * wide, wide), wide)
            o = jnp.dot(attn[mine], ow[:, lanes], preferred_element_type=F32).astype(BF16)
            dst[0, :, lanes] = o[:piece]
            dst[1, :, lanes] = o[piece:]

    def project_all():
        wait_loads("ow", "res", "ng")
        project(1 - core, part)
        for p in (0, 1):
            send(part.at[p], part_in.at[p], p_s.at[p], p_r.at[p], sp, 1 - core)
        project(core, own_part)

    group = 32
    xm, zm = at(1, 0, z), at(0, 0, zmate)
    n_tok = [0]

    def send_tok(src, dst, p, spi, tpi):
        i = n_tok[0]
        n_tok[0] += 1
        rc, c = dst
        send(tok.at[src[0], src[1], p], tok.at[rc, c, p], t_s.at[i], t_r.at[rc, c, p], spi, tpi)

    def to_partner(rc, p):
        send_tok((rc, 0), (rc, 1), p, sp, 1 - core)

    def wait_tok(rc, c, p):
        arrive(tok.at[rc, c, p], t_s.at[0], t_r.at[rc, c, p])

    def middle(p):
        arrive(part_in.at[p], p_s.at[p], p_r.at[p])

        @pl.loop(0, piece // group)
        def _(t):
            rws = pl.ds(pl.multiple_of(t * group, group), group)
            branch = own_part[p, rws].astype(F32) + part_in[p, rws].astype(F32)
            rres = pl.ds(pl.multiple_of(core * half + p * piece + t * group, group), group)
            m = (res[rres].astype(F32) + branch).astype(BF16)
            mid[pl.ds(pl.multiple_of(p * piece + t * group, group), group)] = m
            full = m.astype(F32)
            inv = lax.rsqrt(jnp.mean(full * full, axis=-1, keepdims=True) + EPS)
            tok[0, 0, p, rws] = (full * inv * ng[...]).astype(BF16)

        to_partner(0, p)

    def relay_tok(rc, p, spi):
        wait_tok(rc, 0, p)
        if spi is not None:
            send_tok((rc, 0), (3, 0), p, spi, core)
        to_partner(rc, p)

    waited = set()

    def wait_near(w, dx, k):
        if (dx or k) and (w, dx, k) not in waited:
            waited.add((w, dx, k))
            wait_weight(w, dx, 0, zs[k])

    def block_of(dy, zz):
        block = (zz * 2 + (y + dy) % 2) * 2
        return block, pl.ds(pl.multiple_of(block * depth, pair), pair)

    def raise_first(rc):
        if rc == 0:
            own[0].wait()
        for p in (0, 1):
            wait_tok(rc, 1, p)
        total = None
        for zz in range(4):
            block, feats = block_of(0, zz)
            tokens = tok[rc, :, :, :, feats].reshape(rows, pair)
            w = wup[pl.ds(block, 2)].reshape(pair, cols)
            term = jnp.dot(tokens, w, preferred_element_type=F32)
            total = term if total is None else total + term
        racc[rc] = total

    def raise_second():
        for zz in zs:
            for dx in (0, 1):
                wait_weight(0, dx, 1, zz)

        @pl.loop(0, cols // tile)
        def _(t):
            lanes = pl.ds(pl.multiple_of(t * tile, tile), tile)
            total = racc[:, :, lanes].reshape(4 * rows, tile)
            for zz in range(4):
                block, feats = block_of(1, zz)
                tokens = tok[:, :, :, :, feats].reshape(4 * rows, pair)
                w = wup[pl.ds(block, 2), :, lanes].reshape(pair, tile)
                total = total + jnp.dot(tokens, w, preferred_element_type=F32)
            raised = jnp.square(jnp.maximum(total, 0.0)).astype(BF16)
            hidden[:, :, lanes] = raised.reshape(4, rows, tile)

    def lower(j):
        dy, k = CHUNKS[j]
        zz = zc[k]
        if dy:
            for dx in (0, 1):
                wait_weight(1, dx, 1, zz)
        elif k == 0:
            own[1].wait()
        block = (zz * 2 + (y + dy) % 2) * 2
        w = wdown[pl.ds(block, 2)].reshape(pair, cols)
        for rc in range(4):
            o = lax.dot_general(hidden[rc], w, NT, preferred_element_type=F32).astype(BF16)
            outs[j, 0, rc] = o[:half]
            outs[j, 1, rc] = o[half:]
        send(outs.at[j, 1], outs_in.at[j], o_s.at[j], o_r.at[j], sp, 1 - core)

    def merged(j, rc):
        return outs[j, 0, rc].astype(F32) + outs_in[j, rc].astype(F32)

    def combine(j):
        arrive(outs_in.at[j], o_s.at[j], o_r.at[j])
        for i, rc in ((0, 1), (1, 3)):
            sums[j, i] = merged(j, rc).astype(BF16)
        if j < STRAIGHT:
            both = pl.ds(0, 2)
            send(sums.at[j, both], final_in.at[j, both], f_s.at[j, 0], f_r.at[j, 0], xm, core)
            return
        sums[j, 2] = merged(j, 2).astype(BF16)
        for i, mate in ((1, at(1, 0, zmate)), (0, xm), (2, zm)):
            send(sums.at[j, i], final_in.at[j, i], f_s.at[j, i], f_r.at[j, i], mate, core)

    def combine_z(j):
        if j >= STRAIGHT:
            return
        both = pl.ds(0, 2)
        arrive(final_in.at[j, both], f_s.at[j, 0], f_r.at[j, 0])
        sums[j, 2] = (merged(j, 2) + final_in[j, 1].astype(F32)).astype(BF16)
        send(sums.at[j, 2], final_in.at[j, 2], f_s.at[j, 2], f_r.at[j, 2], zm, core)

    def finish(j):
        dy, k = CHUNKS[j]
        zz = zc[k]
        block = (zz * 2 + (y + dy) % 2) * 2
        total = merged(j, 0)
        if j >= STRAIGHT:
            for i in (0, 1):
                arrive(final_in.at[j, i], f_s.at[j, i], f_r.at[j, i])
                total += final_in[j, i].astype(F32)
        else:
            total += final_in[j, 0].astype(F32)
        arrive(final_in.at[j, 2], f_s.at[j, 2], f_r.at[j, 2])
        total += final_in[j, 2].astype(F32)
        lanes = pl.ds(pl.multiple_of(block * depth, pair), pair)
        out_ref[:, lanes] = (mid[:, lanes].astype(F32) + total).astype(BF16)

    def step(op):
        kind, code = op[0], [int(c) for c in op[1:]]
        if kind == "n":
            send_weight(*code)
        elif kind == "m":
            send_weight_if(inner, *code)
            send_weight(*code, False)
        elif kind == "e":
            send_weight_if(jnp.logical_not(inner), *code)
        elif kind == "f":
            wait_near(*code)
            pass_weight(*code, True)
        elif kind == "y":
            wait_near(*code)
            pass_weight(*code, False)
        elif kind == "K":
            relay_z(code[0])
        elif kind == "R":
            (relay_x if code[0] else relay_y)()
        elif kind == "A":
            dx, dy = ((0, 0), (1, 0), (0, 1), (1, 1))[code[0]]
            attend_column(dx, dy, ((), (2, 3), (0, 1), (0, 1, 2, 3))[code[0]])
        elif kind == "P":
            attention_out()
            project_all()
        elif kind == "M":
            middle(code[0])
        elif kind == "x":
            send_tok((0, 0), (1, 0), code[0], xm, core)
        elif kind == "z":
            send_tok((0, 0), (2, 0), code[0], zm, core)
        elif kind == "r":
            rc, p = code
            relay_tok(rc, p, zm if (rc, p) == (1, 0) else xm if (rc, p) == (2, 1) else None)
        elif kind == "U":
            raise_first(code[0])
        elif kind == "V":
            raise_second()
        elif kind == "L":
            lower(code[0])
        elif kind == "C":
            combine(code[0])
        elif kind == "Z":
            combine_z(code[0])
        elif kind == "F":
            finish(code[0])

    for op in SCHEDULE:
        step(op)

    for c in sent:
        c.wait_send()
    for cond, c in sometimes:
        pl.when(cond)(c.wait_send)


def fused_body(
    queries, keys, values, documents, query_gain, key_gain, out_weight, residual, norm_gain,
    up_weight, down_weight,
):
    rows, heads, width = queries.shape
    n_sp = lax.axis_size("sp")
    model = residual.shape[1]
    depth, cols = up_weight.shape[0], up_weight.shape[1] // 4
    half = rows // 2
    piece = half // 2
    pair = 2 * depth
    chunks = model // pair
    dma = pltpu.SemaphoreType.DMA
    vmem = pltpu.VMEM
    tables = rope_tables(n_sp * rows // GRID, width)
    operands = (
        queries, keys, values, documents[None, :], query_gain[None, :], key_gain[None, :],
        out_weight, residual, norm_gain[None, :], up_weight, down_weight, *tables,
    )
    loaded = [a for i, a in enumerate(operands) if i not in (9, 10)]
    return pl.pallas_call(
        layer_kernel,
        out_shape=jax.ShapeDtypeStruct((half, model), BF16),
        in_specs=[pl.BlockSpec(memory_space=pl.ANY)] * len(operands),
        out_specs=pl.BlockSpec(memory_space=pltpu.VMEM),
        scratch_shapes=[vmem(a.shape, a.dtype) for a in loaded] + [
            vmem((heads, rows, width), BF16),
            vmem((n_sp, 2 * rows + 16, width), BF16),
            vmem((rows, width), F32),
            vmem((rows, 4 * rows), F32),
            vmem((heads * rows, width), F32),
            vmem((heads * rows, width), F32),
            vmem((heads * rows, width), F32),
            vmem((rows, heads * width), BF16),
            vmem((n_sp, depth, cols), BF16),
            vmem((n_sp, depth, cols), BF16),
            vmem((2, piece, model), BF16),
            vmem((2, piece, model), BF16),
            vmem((2, piece, model), BF16),
            vmem((half, model), BF16),
            vmem((4, 2, 2, piece, model), BF16),
            vmem((4, rows, cols), F32),
            vmem((4, rows, cols), BF16),
            vmem((chunks, 2, 4, half, pair), BF16),
            vmem((chunks, 4, half, pair), BF16),
            vmem((chunks, 3, half, pair), BF16),
            vmem((chunks, 3, half, pair), BF16),
            dma((13,)), dma((2,)), dma((17,)), dma((n_sp,)), dma((2, 24)), dma((2, n_sp)),
            dma((2,)), dma((2,)), dma((16,)), dma((4, 2, 2)), dma((chunks,)), dma((chunks,)),
            dma((chunks, 3)), dma((chunks, 3)),
        ],
        compiler_params=pltpu.CompilerParams(
            collective_id=0, has_side_effects=True, vmem_limit_bytes=60 * 1024 * 1024
        ),
    )(*operands)


def solution(mesh):
    in_specs = (
        P("sp", "tp", None),
        P("sp", None, None),
        P("sp", None, None),
        P("sp"),
        P(),
        P(),
        P("tp", None),
        P("sp", None),
        P(),
        P("sp", "tp"),
        P("sp", "tp"),
    )
    out_specs = P(("sp", "tp"), None)
    fused = mesh.shape["tp"] == 2 and mesh.shape["sp"] == 16
    return jax.shard_map(fused_body if fused else body, mesh=mesh, in_specs=in_specs, out_specs=out_specs, check_vma=False)
```

```python
import functools

import jax
import jax.numpy as jnp
import numpy as np
from jax import lax
from jax.experimental import pallas as pl
from jax.experimental.pallas import tpu as pltpu
from jax.sharding import PartitionSpec as P

QUERY_HEADS = 8
GRID = 64


EPS = 1e-06
THETA = 10000.0


def head_norm(block, gain):
    return block * lax.rsqrt(jnp.mean(block * block, axis=-1, keepdims=True) + EPS) * gain


def rotate(block, positions):
    head_width = block.shape[-1]
    pair_count = head_width // 4
    inverse = THETA ** (-jnp.arange(pair_count, dtype=jnp.float32) / pair_count)
    grid_row = (positions // GRID).astype(jnp.float32)[:, None] * inverse
    grid_col = (positions % GRID).astype(jnp.float32)[:, None] * inverse
    angles = jnp.concatenate([grid_row, grid_row, grid_col, grid_col], axis=-1)
    cosine = jnp.cos(angles)[:, None, :]
    sine_table = jnp.sin(angles)[:, None, :]
    turned = jnp.concatenate(
        [
            -block[..., pair_count : 2 * pair_count],
            block[..., 0:pair_count],
            -block[..., 3 * pair_count :],
            block[..., 2 * pair_count : 3 * pair_count],
        ],
        axis=-1,
    )
    return block * cosine + turned * sine_table


def channel_norm(rows_in, gain):
    widened = rows_in.astype(jnp.float32)
    return (
        widened * lax.rsqrt(jnp.mean(widened * widened, axis=-1, keepdims=True) + EPS) * gain
    ).astype(jnp.bfloat16)


def body(
    queries,
    keys,
    values,
    documents,
    query_gain,
    key_gain,
    out_weight,
    residual,
    norm_gain,
    up_weight,
    down_weight,
):
    tok_dev = queries.shape[0]
    heads_here = queries.shape[1]
    head_width = queries.shape[2]
    query_group_count = QUERY_HEADS // keys.shape[1]
    kv_index = lax.axis_index("tp") * heads_here // query_group_count
    positions = lax.axis_index("sp") * tok_dev + jnp.arange(tok_dev, dtype=jnp.int32)
    own_keys = lax.dynamic_index_in_dim(keys, kv_index, 1, keepdims=True)
    own_values = lax.dynamic_index_in_dim(values, kv_index, 1, keepdims=False)
    key_rot = rotate(head_norm(own_keys.astype(jnp.float32), key_gain), positions)[:, 0, :].astype(
        jnp.bfloat16
    )
    rotated_query = rotate(head_norm(queries.astype(jnp.float32), query_gain), positions).astype(
        jnp.bfloat16
    )
    scale = head_width ** (-0.5)
    first_doc = documents[0]
    last_doc = documents[tok_dev - 1]
    start_state = (
        jnp.full((tok_dev, heads_here), -1e30, jnp.float32),
        jnp.zeros((tok_dev, heads_here), jnp.float32),
        jnp.zeros((tok_dev, heads_here, head_width), jnp.float32),
    )
    piece_keys = lax.all_gather(key_rot, "sp", axis=0, tiled=True)
    piece_values = lax.all_gather(own_values, "sp", axis=0, tiled=True)
    piece_docs = lax.all_gather(documents, "sp", axis=0, tiled=True)

    def update(state):
        peak, denom, summed = state
        scores = (
            jnp.einsum("qhd,kd->qhk", rotated_query, piece_keys, preferred_element_type=jnp.float32)
            * scale
        )
        allowed = (documents[:, None] == piece_docs[None, :])[:, None, :]
        scores = jnp.where(allowed, scores, -1e30)
        new_peak = jnp.maximum(peak, jnp.max(scores, axis=-1))
        probs = jnp.where(allowed, jnp.exp(scores - new_peak[..., None]), 0.0)
        denom = jnp.sum(probs, axis=-1)
        summed = jnp.einsum(
            "qhk,kd->qhd",
            probs.astype(jnp.bfloat16),
            piece_values,
            preferred_element_type=jnp.float32,
        )
        return (new_peak, denom, summed)

    touches = jnp.logical_and(
        piece_docs[0] <= last_doc, piece_docs[piece_docs.shape[0] - 1] >= first_doc
    )
    peak, denom, summed = lax.cond(touches, update, lambda state: state, start_state)
    attn = (
        (summed / denom[..., None]).reshape(tok_dev, heads_here * head_width).astype(jnp.bfloat16)
    )
    share = tok_dev // lax.axis_size("tp")
    branch = lax.psum(
        jnp.dot(attn, out_weight, preferred_element_type=jnp.float32).astype(jnp.bfloat16), "tp"
    ).astype(jnp.float32)
    whole_rows = (residual.astype(jnp.float32) + branch).astype(jnp.bfloat16)
    normed = channel_norm(whole_rows, norm_gain)
    mid = lax.dynamic_slice_in_dim(whole_rows, lax.axis_index("tp") * share, share, 0)
    raised = jnp.dot(
        normed,
        lax.all_gather(up_weight, "sp", axis=0, tiled=True),
        preferred_element_type=jnp.float32,
    )
    hidden = jnp.square(jax.nn.relu(raised)).astype(jnp.bfloat16)
    terms = lax.dot_general(
        hidden,
        lax.all_gather(down_weight, "sp", axis=0, tiled=True),
        (((1,), (1,)), ((), ())),
        preferred_element_type=jnp.float32,
    )
    mixer = lax.psum_scatter(
        terms.astype(jnp.bfloat16), "tp", scatter_dimension=0, tiled=True
    ).astype(jnp.float32)
    return (mid.astype(jnp.float32) + mixer).astype(jnp.bfloat16)


MESH = pl.DeviceIdType.MESH
NT = (((1,), (1,)), ((), ()))
F32 = jnp.float32
BF16 = jnp.bfloat16


NEG = -1e30
CHUNKS = ((0, 0), (0, 1), (1, 0), (0, 2), (1, 1), (0, 3), (1, 2), (1, 3))
STRAIGHT = 0
SCHEDULE = (
    "K1", "K2", "K3", "n001", "n002", "n003", "A0", "R0", "R1", "A1",
    "A2", "y000", "n010", "n011", "n012", "n013", "A3", "y001", "P0", "M0",
    "x0", "M1", "z1", "z0", "x1", "n110", "n101", "n111", "m102", "m112",
    "m103", "m113", "y010", "y011", "r10", "r21", "e102", "e112", "e103", "e113",
    "y002", "y012", "y003", "y013", "y100", "U0", "r11", "r20", "U1", "U2",
    "y110", "y101", "y111", "r30", "r31", "U3", "V0", "L0", "C0", "L1",
    "C1", "y102", "y112", "L2", "C2", "Z0", "L3", "C3", "Z1", "y103",
    "y113", "L4", "C4", "Z2", "F0", "L5", "C5", "Z3", "F1", "L6",
    "C6", "Z4", "F2", "L7", "C7", "Z5", "Z6", "Z7", "F3", "F4",
    "F5", "F6", "F7",
)


def rope_tables(n_rows, width):
    quarter = width // 4
    steps = np.arange(quarter, dtype=np.float32) / np.float32(quarter)
    inverse = (np.float32(THETA) ** (-steps)).astype(np.float32)
    tables = []
    for f in (np.cos, np.sin):
        row, col = np.zeros((n_rows, width), np.float32), np.zeros((GRID, width), np.float32)
        for table, at in ((row, 0), (col, 2 * quarter)):
            angle = np.arange(table.shape[0], dtype=np.float32)[:, None] * inverse
            value = f(angle.astype(np.float64))
            table[:, at : at + quarter] = -value if f is np.sin else value
            table[:, at + quarter : at + 2 * quarter] = value
        tables += [row, col]
    return tables


def layer_kernel(
    q_hbm, k_hbm, v_hbm, doc_hbm, qg_hbm, kg_hbm, ow_hbm, res_hbm, ng_hbm, up_hbm, down_hbm,
    cr_hbm, cc_hbm, sr_hbm, sc_hbm, out_ref,
    q_raw, k_raw, v_raw, doc_v, qg, kg, ow, res, ng, cr, cc, sr, sc,
    q_rot, kv_all, dcol, bias, peak_s, den_s, acc_s, attn, wup, wdown, part, part_in, own_part,
    mid, tok, racc, hidden, outs, outs_in, sums, final_in,
    ld_s, own_s, kv_s, kv_r, w_s, w_r, p_s, p_r, t_s, t_r, o_s, o_r, f_s, f_r,
):
    rows, heads, width = q_raw.shape
    half = rows // 2
    piece = half // 2
    depth, cols = wup.shape[1], wup.shape[2]
    model = ow.shape[1]
    pair = 2 * depth
    sp, core = lax.axis_index("sp"), lax.axis_index("tp")
    x, y, z = sp % 2, (sp // 2) % 2, sp // 4
    zh = z // 2
    zmate = z + 1 - 2 * (z % 2)
    far = [2 - zh, 3 * (1 - zh)]
    zs = [z, zmate] + far
    zc = [2 * zh, 2 * zh + 1] + far

    def at(dx, dy, zz):
        return (zz * 2 + (y + dy) % 2) * 2 + (x + dx) % 2

    def rank(dx, zz):
        return zz % 2 * 2 + (x + dx) % 2

    sent = []

    def send(src, dst, ss, rs, spi, tpi, start=True):
        c = pltpu.make_async_remote_copy(
            src_ref=src, dst_ref=dst, send_sem=ss, recv_sem=rs,
            device_id=(spi, tpi), device_id_type=MESH,
        )
        if start:
            c.start()
        sent.append(c)

    def arrive(dst, ss, rs):
        pltpu.make_async_remote_copy(
            src_ref=dst, dst_ref=dst, send_sem=ss, recv_sem=rs,
            device_id=(sp, 1 - core), device_id_type=MESH,
        ).wait_recv()

    loads = {}
    for i, (name, src, dst) in enumerate([
        ("k", k_hbm, k_raw), ("v", v_hbm, v_raw), ("doc", doc_hbm, doc_v), ("kg", kg_hbm, kg),
        ("cr", cr_hbm, cr), ("cc", cc_hbm, cc), ("sr", sr_hbm, sr), ("sc", sc_hbm, sc),
        ("q", q_hbm, q_raw), ("qg", qg_hbm, qg), ("ow", ow_hbm, ow), ("res", res_hbm, res),
        ("ng", ng_hbm, ng),
    ]):
        loads[name] = pltpu.make_async_copy(src, dst, ld_s.at[i])
        loads[name].start()
    weights = ((up_hbm, wup), (down_hbm, wdown))

    def columns(w, dx, zz):
        return weights[w][0].at[:, pl.ds(pl.multiple_of(rank(dx, zz) * cols, 128), cols)]

    own = []
    for w in (0, 1):
        own.append(pltpu.make_async_copy(columns(w, 0, z), weights[w][1].at[sp], own_s.at[w]))
        own[w].start()

    barrier = pltpu.get_barrier_semaphore()
    peers = [(at(0, 0, zz), core) for zz in zs[1:]]
    peers += [(at(1, 0, z), core), (at(1, 0, zmate), core), (at(0, 1, z), core), (sp, 1 - core)]
    for p in peers:
        pl.semaphore_signal(barrier, inc=1, device_id=p, device_id_type=MESH)

    def wait_loads(*names):
        for name in names:
            loads[name].wait()

    wait_loads("k", "v", "doc", "kg", "cr", "cc", "sr", "sc")
    grid_rows = rows // GRID

    def table(row, col):
        lines = row[pl.ds(sp * grid_rows, grid_rows)]
        return (lines[:, None, :] + col[...][None]).reshape(rows, width)

    cosine, sine = table(cr, cc), table(sr, sc)
    first = lax.broadcasted_iota(jnp.int32, (rows, width), 1) % (width // 2) < width // 4

    def norm_rope(v, gain):
        v = v * lax.rsqrt(jnp.mean(v * v, axis=-1, keepdims=True) + EPS) * gain[...]
        turned = jnp.where(
            first, pltpu.roll(v, width - width // 4, 1), pltpu.roll(v, width // 4, 1)
        )
        return (v * cosine + turned * sine).astype(BF16)

    def own_head(ref):
        both = ref[...].astype(F32)
        return jnp.where(core == 0, both[:, 0, :], both[:, 1, :])

    kv_all[sp, 0:rows] = norm_rope(own_head(k_raw), kg)
    kv_all[sp, rows : 2 * rows] = own_head(v_raw).astype(BF16)
    docs = doc_v[...].astype(F32)
    lines = [docs[:, i * width : (i + 1) * width] for i in range(rows // width)]
    pad = kv_all.shape[1] - 2 * rows - len(lines)
    lines.append(jnp.zeros((pad, width), F32))
    kv_all[sp, 2 * rows :] = jnp.concatenate(lines, axis=0).astype(BF16)

    pl.semaphore_wait(barrier, len(peers))

    def send_kv(i, slot, spi):
        send(kv_all.at[slot], kv_all.at[slot], kv_s.at[i], kv_r.at[slot], spi, core)

    def wait_kv(slot):
        arrive(kv_all.at[slot], kv_s.at[0], kv_r.at[slot])

    def send_weight(w, dx, k, start=True):
        send(
            columns(w, dx, zs[k]), weights[w][1].at[sp],
            w_s.at[w, dx * 4 + k], w_r.at[w, sp], at(dx, 0, zs[k]), core, start,
        )

    def send_weight_if(cond, w, dx, k):
        count = len(sent)
        pl.when(cond)(lambda: send_weight(w, dx, k))
        del sent[count:]

    def wait_weight(w, dx, dy, zz):
        i = at(dx, dy, zz)
        arrive(weights[w][1].at[i], w_s.at[w, 0], w_r.at[w, i])

    def pass_weight(w, dx, k, across):
        i = at(dx, 0, zs[k])
        dst = weights[w][1]
        src = dst.at[i] if dx or k else columns(w, 0, z)
        send(
            src, dst.at[i], w_s.at[w, (16 if across else 8) + dx * 4 + k], w_r.at[w, i],
            at(0, 0, (z + 2) % 4) if across else at(0, 1, z), core,
        )

    for k in (1, 2, 3):
        send_kv(k, sp, at(0, 0, zs[k]))
    send_kv(0, sp, at(1, 0, z))
    send_kv(4, sp, at(0, 1, z))

    wait_loads("q", "qg")
    wide = q_raw[...].astype(F32)
    for h in range(heads):
        q_rot[h] = norm_rope(wide[:, h, :], qg)
    dcol[...] = jnp.broadcast_to(docs, (width, rows)).T

    for h in range(heads):
        lines = pl.ds(h * rows, rows)
        peak_s[lines] = jnp.full((rows, width), NEG, F32)
        den_s[lines] = jnp.zeros((rows, width), F32)
        acc_s[lines] = jnp.zeros((rows, width), F32)
    scale = float(width ** (-0.5) * np.log2(np.e))
    tiles = rows // width

    def attend(slots):
        for b, i in enumerate(slots):
            theirs = kv_all[i, 2 * rows :].astype(F32)
            for t in range(tiles):
                bias[:, (b * tiles + t) * width : (b * tiles + t + 1) * width] = jnp.where(
                    dcol[...] == theirs[t : t + 1], 0.0, NEG
                )
        for h in range(heads):
            lines = pl.ds(h * rows, rows)
            scores = []
            for b, i in enumerate(slots):
                s = lax.dot_general(
                    q_rot[h], kv_all[i, 0:rows], NT, preferred_element_type=F32
                )
                scores.append(s * scale + bias[:, b * rows : (b + 1) * rows])
            top = functools.reduce(
                jnp.maximum,
                [s[:, t * width : (t + 1) * width] for s in scores for t in range(tiles)],
            )
            peak = peak_s[lines]
            new_peak = jnp.maximum(peak, jnp.max(top, axis=-1, keepdims=True))
            peak_s[lines] = new_peak
            decay = jnp.exp2(peak - new_peak)
            spread = jnp.concatenate([new_peak] * tiles, axis=1)
            probs = [jnp.exp2(s - spread) for s in scores]
            den_s[lines] = den_s[lines] * decay + functools.reduce(
                jnp.add,
                [p[:, t * width : (t + 1) * width] for p in probs for t in range(tiles)],
            )
            acc_s[lines] = acc_s[lines] * decay + functools.reduce(
                jnp.add,
                [
                    jnp.dot(p.astype(BF16), kv_all[i, rows : 2 * rows], preferred_element_type=F32)
                    for i, p in zip(slots, probs)
                ],
            )

    def column(dx, dy):
        return [at(dx, dy, zz) for zz in zs]

    def relay_z(k):
        i = at(0, 0, zs[k])
        wait_kv(i)
        send_kv(4 + k, i, at(1, 0, z))
        send_kv(8 + k, i, at(0, 1, z))

    def relay_y():
        for k in (0, 1):
            i = at(1, 0, zs[k])
            wait_kv(i)
            send_kv(12 + k, i, at(0, 1, z))

    def relay_x():
        for k in (2, 3):
            i = at(0, 1, zs[k])
            wait_kv(i)
            send_kv(12 + k, i, at(1, 0, z))

    def attend_column(dx, dy, ks):
        for k in ks:
            wait_kv(at(dx, dy, zs[k]))
        attend(column(dx, dy))

    def attention_out():
        for h in range(heads):
            lines = pl.ds(h * rows, rows)
            denom = jnp.sum(den_s[lines], axis=-1, keepdims=True)
            attn[:, h * width : (h + 1) * width] = (acc_s[lines] / denom).astype(BF16)

    tile = 256

    def project(owner, dst):
        mine = pl.ds(pl.multiple_of(owner * half, half), half)
        wide = 4 * tile

        @pl.loop(0, model // wide)
        def _(t):
            lanes = pl.ds(pl.multiple_of(t * wide, wide), wide)
            o = jnp.dot(attn[mine], ow[:, lanes], preferred_element_type=F32).astype(BF16)
            dst[0, :, lanes] = o[:piece]
            dst[1, :, lanes] = o[piece:]

    def project_all():
        wait_loads("ow", "res", "ng")
        project(1 - core, part)
        for p in (0, 1):
            send(part.at[p], part_in.at[p], p_s.at[p], p_r.at[p], sp, 1 - core)
        project(core, own_part)

    group = 32
    xm, zm = at(1, 0, z), at(0, 0, zmate)
    n_tok = [0]

    def send_tok(src, dst, p, spi, tpi):
        i = n_tok[0]
        n_tok[0] += 1
        rc, c = dst
        send(tok.at[src[0], src[1], p], tok.at[rc, c, p], t_s.at[i], t_r.at[rc, c, p], spi, tpi)

    def to_partner(rc, p):
        send_tok((rc, 0), (rc, 1), p, sp, 1 - core)

    def wait_tok(rc, c, p):
        arrive(tok.at[rc, c, p], t_s.at[0], t_r.at[rc, c, p])

    def middle(p):
        arrive(part_in.at[p], p_s.at[p], p_r.at[p])

        @pl.loop(0, piece // group)
        def _(t):
            rws = pl.ds(pl.multiple_of(t * group, group), group)
            branch = own_part[p, rws].astype(F32) + part_in[p, rws].astype(F32)
            rres = pl.ds(pl.multiple_of(core * half + p * piece + t * group, group), group)
            m = (res[rres].astype(F32) + branch).astype(BF16)
            mid[pl.ds(pl.multiple_of(p * piece + t * group, group), group)] = m
            full = m.astype(F32)
            inv = lax.rsqrt(jnp.mean(full * full, axis=-1, keepdims=True) + EPS)
            tok[0, 0, p, rws] = (full * inv * ng[...]).astype(BF16)

        to_partner(0, p)

    def relay_tok(rc, p, spi):
        wait_tok(rc, 0, p)
        if spi is not None:
            send_tok((rc, 0), (3, 0), p, spi, core)
        to_partner(rc, p)

    waited = set()
    inner = (z == 1) | (z == 2)

    def wait_near(w, dx, k):
        if (dx or k) and (w, dx, k) not in waited:
            waited.add((w, dx, k))
            wait_weight(w, dx, 0, zs[k])

    def block_of(dy, zz):
        block = (zz * 2 + (y + dy) % 2) * 2
        return block, pl.ds(pl.multiple_of(block * depth, pair), pair)

    def raise_first(rc):
        if rc == 0:
            own[0].wait()
        for p in (0, 1):
            wait_tok(rc, 1, p)
        total = None
        for zz in range(4):
            block, feats = block_of(0, zz)
            tokens = tok[rc, :, :, :, feats].reshape(rows, pair)
            w = wup[pl.ds(block, 2)].reshape(pair, cols)
            term = jnp.dot(tokens, w, preferred_element_type=F32)
            total = term if total is None else total + term
        racc[rc] = total

    def raise_second():
        for zz in zs:
            for dx in (0, 1):
                wait_weight(0, dx, 1, zz)

        @pl.loop(0, cols // tile)
        def _(t):
            lanes = pl.ds(pl.multiple_of(t * tile, tile), tile)
            total = racc[:, :, lanes].reshape(4 * rows, tile)
            for zz in range(4):
                block, feats = block_of(1, zz)
                tokens = tok[:, :, :, :, feats].reshape(4 * rows, pair)
                w = wup[pl.ds(block, 2), :, lanes].reshape(pair, tile)
                total = total + jnp.dot(tokens, w, preferred_element_type=F32)
            raised = jnp.square(jnp.maximum(total, 0.0)).astype(BF16)
            hidden[:, :, lanes] = raised.reshape(4, rows, tile)

    def lower(j):
        dy, k = CHUNKS[j]
        zz = zc[k]
        if dy:
            for dx in (0, 1):
                wait_weight(1, dx, 1, zz)
        elif k == 0:
            own[1].wait()
        block = (zz * 2 + (y + dy) % 2) * 2
        w = wdown[pl.ds(block, 2)].reshape(pair, cols)
        for rc in range(4):
            o = lax.dot_general(hidden[rc], w, NT, preferred_element_type=F32).astype(BF16)
            outs[j, 0, rc] = o[:half]
            outs[j, 1, rc] = o[half:]
        send(outs.at[j, 1], outs_in.at[j], o_s.at[j], o_r.at[j], sp, 1 - core)

    def merged(j, rc):
        return outs[j, 0, rc].astype(F32) + outs_in[j, rc].astype(F32)

    def combine(j):
        arrive(outs_in.at[j], o_s.at[j], o_r.at[j])
        for i, rc in ((0, 1), (1, 3)):
            sums[j, i] = merged(j, rc).astype(BF16)
        if j < STRAIGHT:
            both = pl.ds(0, 2)
            send(sums.at[j, both], final_in.at[j, both], f_s.at[j, 0], f_r.at[j, 0], xm, core)
            return
        sums[j, 2] = merged(j, 2).astype(BF16)
        for i, mate in ((1, at(1, 0, zmate)), (0, xm), (2, zm)):
            send(sums.at[j, i], final_in.at[j, i], f_s.at[j, i], f_r.at[j, i], mate, core)

    def combine_z(j):
        if j >= STRAIGHT:
            return
        both = pl.ds(0, 2)
        arrive(final_in.at[j, both], f_s.at[j, 0], f_r.at[j, 0])
        sums[j, 2] = (merged(j, 2) + final_in[j, 1].astype(F32)).astype(BF16)
        send(sums.at[j, 2], final_in.at[j, 2], f_s.at[j, 2], f_r.at[j, 2], zm, core)

    def finish(j):
        dy, k = CHUNKS[j]
        zz = zc[k]
        block = (zz * 2 + (y + dy) % 2) * 2
        total = merged(j, 0)
        if j >= STRAIGHT:
            for i in (0, 1):
                arrive(final_in.at[j, i], f_s.at[j, i], f_r.at[j, i])
                total += final_in[j, i].astype(F32)
        else:
            total += final_in[j, 0].astype(F32)
        arrive(final_in.at[j, 2], f_s.at[j, 2], f_r.at[j, 2])
        total += final_in[j, 2].astype(F32)
        lanes = pl.ds(pl.multiple_of(block * depth, pair), pair)
        out_ref[:, lanes] = (mid[:, lanes].astype(F32) + total).astype(BF16)

    def step(op):
        kind, code = op[0], [int(c) for c in op[1:]]
        if kind == "n":
            send_weight(*code)
        elif kind == "m":
            send_weight_if(inner, *code)
            send_weight(*code, False)
        elif kind == "e":
            send_weight_if(jnp.logical_not(inner), *code)
        elif kind == "f":
            wait_near(*code)
            pass_weight(*code, True)
        elif kind == "y":
            wait_near(*code)
            pass_weight(*code, False)
        elif kind == "K":
            relay_z(code[0])
        elif kind == "R":
            (relay_x if code[0] else relay_y)()
        elif kind == "A":
            dx, dy = ((0, 0), (1, 0), (0, 1), (1, 1))[code[0]]
            attend_column(dx, dy, ((), (2, 3), (0, 1), (0, 1, 2, 3))[code[0]])
        elif kind == "P":
            attention_out()
            project_all()
        elif kind == "M":
            middle(code[0])
        elif kind == "x":
            send_tok((0, 0), (1, 0), code[0], xm, core)
        elif kind == "z":
            send_tok((0, 0), (2, 0), code[0], zm, core)
        elif kind == "r":
            rc, p = code
            relay_tok(rc, p, zm if (rc, p) == (1, 0) else xm if (rc, p) == (2, 1) else None)
        elif kind == "U":
            raise_first(code[0])
        elif kind == "V":
            raise_second()
        elif kind == "L":
            lower(code[0])
        elif kind == "C":
            combine(code[0])
        elif kind == "Z":
            combine_z(code[0])
        elif kind == "F":
            finish(code[0])

    for op in SCHEDULE:
        step(op)

    for c in sent:
        c.wait_send()


def fused_body(
    queries, keys, values, documents, query_gain, key_gain, out_weight, residual, norm_gain,
    up_weight, down_weight,
):
    rows, heads, width = queries.shape
    n_sp = lax.axis_size("sp")
    model = residual.shape[1]
    depth, cols = up_weight.shape[0], up_weight.shape[1] // 4
    half = rows // 2
    piece = half // 2
    pair = 2 * depth
    chunks = model // pair
    dma = pltpu.SemaphoreType.DMA
    vmem = pltpu.VMEM
    tables = rope_tables(n_sp * rows // GRID, width)
    operands = (
        queries, keys, values, documents[None, :], query_gain[None, :], key_gain[None, :],
        out_weight, residual, norm_gain[None, :], up_weight, down_weight, *tables,
    )
    loaded = [a for i, a in enumerate(operands) if i not in (9, 10)]
    return pl.pallas_call(
        layer_kernel,
        out_shape=jax.ShapeDtypeStruct((half, model), BF16),
        in_specs=[pl.BlockSpec(memory_space=pl.ANY)] * len(operands),
        out_specs=pl.BlockSpec(memory_space=pltpu.VMEM),
        scratch_shapes=[vmem(a.shape, a.dtype) for a in loaded] + [
            vmem((heads, rows, width), BF16),
            vmem((n_sp, 2 * rows + 16, width), BF16),
            vmem((rows, width), F32),
            vmem((rows, 4 * rows), F32),
            vmem((heads * rows, width), F32),
            vmem((heads * rows, width), F32),
            vmem((heads * rows, width), F32),
            vmem((rows, heads * width), BF16),
            vmem((n_sp, depth, cols), BF16),
            vmem((n_sp, depth, cols), BF16),
            vmem((2, piece, model), BF16),
            vmem((2, piece, model), BF16),
            vmem((2, piece, model), BF16),
            vmem((half, model), BF16),
            vmem((4, 2, 2, piece, model), BF16),
            vmem((4, rows, cols), F32),
            vmem((4, rows, cols), BF16),
            vmem((chunks, 2, 4, half, pair), BF16),
            vmem((chunks, 4, half, pair), BF16),
            vmem((chunks, 3, half, pair), BF16),
            vmem((chunks, 3, half, pair), BF16),
            dma((13,)), dma((2,)), dma((16,)), dma((n_sp,)), dma((2, 24)), dma((2, n_sp)),
            dma((2,)), dma((2,)), dma((16,)), dma((4, 2, 2)), dma((chunks,)), dma((chunks,)),
            dma((chunks, 3)), dma((chunks, 3)),
        ],
        compiler_params=pltpu.CompilerParams(
            collective_id=0, has_side_effects=True, vmem_limit_bytes=60 * 1024 * 1024
        ),
    )(*operands)


def solution(mesh):
    in_specs = (
        P("sp", "tp", None),
        P("sp", None, None),
        P("sp", None, None),
        P("sp"),
        P(),
        P(),
        P("tp", None),
        P("sp", None),
        P(),
        P("sp", "tp"),
        P("sp", "tp"),
    )
    out_specs = P(("sp", "tp"), None)
    fused = mesh.shape["tp"] == 2 and mesh.shape["sp"] == 16
    return jax.shard_map(fused_body if fused else body, mesh=mesh, in_specs=in_specs, out_specs=out_specs, check_vma=False)
```
